512 devices in a mesh: sp: 64 (over z, y), tp: 8 (over x, core).
Axes of the slice: x: 4, y: 4, z: 16, core: 2. Of those that a mesh axis runs over, the one named last changes fastest.
Arguments:
- tokens: bfloat16 [16384, 2048], P('sp', 'tp'), may hold values from -6 to 6
- norm_gain: float32 [2048], replicated, may hold values from 0.1 to 1.9
- query_weight: bfloat16 [1024, 2048], P('tp'), may hold values from -0.125 to 0.125
- key_weight: bfloat16 [1024, 2048], P('tp'), may hold values from -0.125 to 0.125
- value_weight: bfloat16 [1024, 2048], P('tp'), may hold values from -0.125 to 0.125
- pool_weight: bfloat16 [1024, 2048], P('tp'), may hold values from -0.125 to 0.125
- query_gain: float32 [64], replicated, may hold values from 0.6 to 6
- key_gain: float32 [64], replicated, may hold values from 0.6 to 6
- cum_gate: float32 [16384, 16], P('sp', 'tp'), as said below
- out_pool_weight: bfloat16 [1024, 2048], P(None, 'tp'), may hold values from -0.1875 to 0.1875
- out_attn_weight: bfloat16 [1024, 2048], P(None, 'tp'), may hold values from -0.1875 to 0.1875
Outputs:
- mixed: bfloat16 [16384, 2048], P('sp', 'tp')
The draws below stay inside these ranges and needn't reach their ends.
Inputs may be any that keep to these rules, and one draw needn't show every extreme that they name: `cum_gate`: in each head the values never rise along the positions.
All inputs are finite; a program needn't handle non-finite values.
Results may differ from the reference program's by a relative error of at most 0.005.
The reference program's roundings to bfloat16 on the way count: a program that leaves them out, or rounds other values in their place, can miss the bound.
Values may be sent and summed in bfloat16 or wider, within the bound.
No kernel may reach another device: no remote copies, remote signals or barrier semaphores. Data moves between devices by JAX's collectives and lax.ppermute only.
A program may use at most 64 MiB of HBM per device.

```python
import jax
import jax.numpy as jnp
from jax import lax

D = 2048
ATTENTION_HEADS = 16
HEAD_DIM = 64
POOL_WIDTH = 1024
POOL_GROUPS = 4
TOK_DEV = 256
SEQUENCE_TOKENS = 16384
N_SP = 64


def draw_cum_gate(key, part):
    key_sections = jax.random.split(jax.random.fold_in(key, 7), 5)
    ranking = jax.random.permutation(key_sections[0], ATTENTION_HEADS)
    slow_flag = ranking >= ATTENTION_HEADS // 2
    block_count = SEQUENCE_TOKENS // TOK_DEV
    factor = jnp.exp(jax.random.uniform(key_sections[1], (block_count, 1), jnp.float32, -0.7, 0.7))
    factor = jnp.repeat(factor, TOK_DEV, axis=0)
    roughness = jax.random.uniform(key_sections[2], (SEQUENCE_TOKENS, ATTENTION_HEADS), jnp.float32, 0.5, 1.5)
    base_rate = jnp.where(slow_flag, 0.8 / SEQUENCE_TOKENS, 1.0 / 40.0)
    forget_decay = base_rate[None, :] * factor * roughness
    spike_positions = jax.random.randint(key_sections[3], (2, ATTENTION_HEADS), 0, SEQUENCE_TOKENS)
    spike_length = -jnp.log(jax.random.uniform(key_sections[4], (2, ATTENTION_HEADS), jnp.float32, 0.5, 0.8))
    location_list = jnp.arange(SEQUENCE_TOKENS, dtype=jnp.int32)[None, :, None] == spike_positions[:, None, :]
    spike_events = jnp.sum(jnp.where(location_list, spike_length[:, None, :], 0.0), axis=0)
    spike_events = jnp.where(slow_flag[None, :], spike_events, 0.0)
    return -jnp.cumsum(forget_decay + spike_events, axis=0)


def draw_query_gain(key, part):
    sub_key = jax.random.fold_in(key, 11)
    return jax.random.uniform(sub_key, (HEAD_DIM,), jnp.float32, 0.6, 1.4)


def draw_key_gain(key, part):
    sub_key = jax.random.fold_in(key, 12)
    return jax.random.uniform(sub_key, (HEAD_DIM,), jnp.float32, 0.6, 1.4)


def block_scale(rng, dims, cuts, smallest, largest):
    loudness, own = 1.0, jax.random.fold_in(rng, 6)
    for dim, blocks in cuts:
        draws = jnp.exp(jax.random.uniform(jax.random.fold_in(own, dim), (blocks,), jnp.float32, smallest / len(cuts), largest / len(cuts)))
        loudness = loudness * jnp.repeat(draws, dims[dim] // blocks).reshape([-1 if axis == dim else 1 for axis in range(len(dims))])
    return loudness


def gaussian(stream_key, shape, spread, reach, cuts=(), kind=jnp.bfloat16):
    level = block_scale(stream_key, shape, cuts, -0.22, 0.18) if cuts else 1.0
    values = jax.random.normal(stream_key, shape, jnp.float32) * spread * level
    return jnp.minimum(jnp.maximum(values, -reach), reach).astype(kind)


def setup_inputs(seed: int = 0) -> dict:
    seeds = jax.random.split(jax.random.key(seed), 12)
    tokens = gaussian(seeds[0], (SEQUENCE_TOKENS, D), 1.0, 6.0, ((0, 64), (1, 8)))
    norm_gain = jnp.clip(1.0 + 0.18 * jax.random.normal(seeds[1], (D,), jnp.float32), 0.1, 1.9)
    query_weight = gaussian(seeds[2], (ATTENTION_HEADS * HEAD_DIM, D), D ** -0.5, 0.125, ((0, 8),))
    key_weight = gaussian(seeds[3], (ATTENTION_HEADS * HEAD_DIM, D), D ** -0.5, 0.125, ((0, 8),))
    value_weight = gaussian(seeds[4], (ATTENTION_HEADS * HEAD_DIM, D), D ** -0.5, 0.125, ((0, 8),))
    pool_weight = gaussian(seeds[5], (POOL_WIDTH, D), D ** -0.5, 0.125, ((0, 8),))
    query_gain = draw_query_gain(jax.random.fold_in(seeds[11], 71), 0)
    key_gain = draw_key_gain(jax.random.fold_in(seeds[11], 71), 0)
    cum_gate = draw_cum_gate(jax.random.fold_in(seeds[11], 71), 0)
    out_pool_weight = gaussian(seeds[9], (POOL_WIDTH, D), POOL_WIDTH ** -0.5, 0.1875, ((1, 8),))
    out_attn_weight = gaussian(seeds[10], (ATTENTION_HEADS * HEAD_DIM, D), (ATTENTION_HEADS * HEAD_DIM) ** -0.5, 0.1875, ((1, 8),))
    return dict(tokens=tokens, norm_gain=norm_gain, query_weight=query_weight, key_weight=key_weight, value_weight=value_weight, pool_weight=pool_weight, query_gain=query_gain, key_gain=key_gain, cum_gate=cum_gate, out_pool_weight=out_pool_weight, out_attn_weight=out_attn_weight)


epsilon = 1e-06
masked_fill = -1e+30

def rms_scale(values, gain):
    return values * lax.rsqrt(lax.optimization_barrier(jnp.mean(values * values, axis=-1, keepdims=True)) + epsilon) * gain

def block_partials(query_rows, query_pos, query_gate, key_rows, value_rows, key_pos, key_gate):
    logits = jnp.einsum('qhd,gkhd->qhgk', query_rows.astype(jnp.float32), key_rows.astype(jnp.float32))
    logits = logits + query_gate[:, :, None, None] - jnp.transpose(key_gate, (2, 0, 1))[None]
    allowed = key_pos[None, None, :, :] <= query_pos[:, None, None, None]
    logits = jnp.where(allowed, logits, masked_fill)
    block_max = lax.optimization_barrier(jnp.max(logits, axis=-1))
    weights = jnp.where(allowed, jnp.exp(logits - block_max[..., None]), 0.0)
    totals = lax.optimization_barrier(jnp.sum(weights, axis=-1))
    rounded = lax.optimization_barrier(weights.astype(jnp.bfloat16))
    numerator = jnp.einsum('qhgk,gkhd->qhgd', rounded.astype(jnp.float32), value_rows.astype(jnp.float32))
    return (block_max, totals, numerator)

def pool_reference(values):
    seq_len = values.shape[0]
    group_width = POOL_WIDTH // POOL_GROUPS
    counts = jnp.arange(1, seq_len + 1, dtype=jnp.int32).astype(jnp.float32)[:, None]
    pieces = []
    for group_index in range(POOL_GROUPS):
        window = 2 ** (group_index + 1)
        column = values[:, group_index * group_width:(group_index + 1) * group_width]
        padded = jnp.pad(column, ((window, 0), (0, 0)))
        running = jnp.zeros_like(column)
        for lag_index in range(window):
            running = running + padded[window - lag_index:window - lag_index + seq_len]
        pieces.append(running / jnp.minimum(counts, float(window)))
    return jnp.concatenate(pieces, axis=1) - values

def reference(tokens, norm_gain, query_weight, key_weight, value_weight, pool_weight, query_gain, key_gain, cum_gate, out_pool_weight, out_attn_weight):
    seq_len = tokens.shape[0]
    normed = rms_scale(tokens.astype(jnp.float32), norm_gain).astype(jnp.bfloat16)

    def project(weight):
        return lax.dot_general(normed, weight, (((1,), (1,)), ((), ())), preferred_element_type=jnp.float32)
    query_all = (rms_scale(project(query_weight).reshape(seq_len, ATTENTION_HEADS, HEAD_DIM), query_gain) * HEAD_DIM ** (-0.5)).astype(jnp.bfloat16)
    key_all = rms_scale(project(key_weight).reshape(seq_len, ATTENTION_HEADS, HEAD_DIM), key_gain).astype(jnp.bfloat16)
    value_all = project(value_weight).astype(jnp.bfloat16).reshape(seq_len, ATTENTION_HEADS, HEAD_DIM)
    pool_input = project(pool_weight).astype(jnp.bfloat16)
    pooled = pool_reference(pool_input.astype(jnp.float32)).astype(jnp.bfloat16)
    key_blocks = key_all.reshape(N_SP, TOK_DEV, ATTENTION_HEADS, HEAD_DIM)
    value_blocks = value_all.reshape(N_SP, TOK_DEV, ATTENTION_HEADS, HEAD_DIM)
    gate_blocks = cum_gate.reshape(N_SP, TOK_DEV, ATTENTION_HEADS)
    positions = jnp.arange(seq_len, dtype=jnp.int32)
    key_pos = positions.reshape(N_SP, TOK_DEV)

    def one_block(index):
        start = (index * TOK_DEV).astype(jnp.int32)
        query_rows = lax.dynamic_slice_in_dim(query_all, start, TOK_DEV, 0)
        query_gate = lax.dynamic_slice_in_dim(cum_gate, start, TOK_DEV, 0)
        query_pos = lax.dynamic_slice_in_dim(positions, start, TOK_DEV, 0)
        block_max, totals, numerator = block_partials(query_rows, query_pos, query_gate, key_blocks, value_blocks, key_pos, gate_blocks)
        top = lax.optimization_barrier(jnp.max(block_max, axis=2, keepdims=True))
        scale = jnp.exp(block_max - top)
        denom = lax.optimization_barrier(jnp.sum(scale * totals, axis=2))
        accum = lax.optimization_barrier(jnp.sum(scale[..., None] * numerator, axis=2))
        return accum / denom[..., None]
    attended = lax.map(one_block, jnp.arange(N_SP, dtype=jnp.int32))
    attended = attended.reshape(seq_len, ATTENTION_HEADS * HEAD_DIM).astype(jnp.bfloat16)
    mixed = jnp.dot(pooled, out_pool_weight, preferred_element_type=jnp.float32) + jnp.dot(attended, out_attn_weight, preferred_element_type=jnp.float32)
    return mixed.astype(jnp.bfloat16)
```

```python
import jax
import jax.numpy as jnp
import numpy as np
from jax import lax
from jax.experimental import pallas as pl
from jax.experimental.pallas import tpu as pltpu
from jax.sharding import Mesh, PartitionSpec as P

F32 = jnp.float32
BF16 = jnp.bfloat16
HEAD = 64
EPS = 1e-06
NEG = -1e30
ROWS = 256
SUB = 32
NZ, NY, NX, NC = 16, 4, 4, 2
TP = ("x", "c")
SP = ("z", "y")


def iota(shape, dim):
    return lax.broadcasted_iota(jnp.int32, shape, dim)


def dot_t(a, b):
    return lax.dot_general(a, b, (((1,), (1,)), ((), ())), preferred_element_type=F32)


def dot(a, b):
    return lax.dot_general(a, b, (((1,), (0,)), ((), ())), preferred_element_type=F32)


def three_parts(v):
    a = v.astype(BF16).astype(F32)
    b = (v - a).astype(BF16).astype(F32)
    return a, b, (v - a - b).astype(BF16).astype(F32)


def head_scale(v, gain, times):
    parts = []
    for h in range(2):
        w = v[:, h * HEAD : (h + 1) * HEAD]
        w = w * lax.rsqrt(jnp.mean(w * w, axis=-1, keepdims=True) + EPS) * gain
        parts.append(w * times if times else w)
    return parts


def project_kernel(
    where, own, other, gain, wq, wk, wv, wp, qg, kg, gate, msg, pool, normed
):
    c = where[0]
    total = jnp.zeros((ROWS, 1), F32)
    for x in range(NX):
        for ref in (own, other):
            v = ref[x].astype(F32)
            total = total + jnp.sum(v * v, axis=-1, keepdims=True)
    scale = lax.rsqrt(total / 2048.0 + EPS)
    for x in range(NX):
        for k, ref in enumerate((own, other)):
            at = pl.multiple_of((2 * x + (c if k == 0 else 1 - c)) * 256, 256)
            v = ref[x].astype(F32) * scale * gain[:, pl.ds(at, 256)]
            normed[:, pl.ds(at, 256)] = v.astype(BF16)
    rows = normed[...]
    q = head_scale(dot_t(rows, wq[...]), qg[...], HEAD ** (-0.5))
    k = head_scale(dot_t(rows, wk[...]), kg[...], None)
    v = dot_t(rows, wv[...])
    pool[...] = dot_t(rows, wp[...]).astype(BF16)
    for h in range(2):
        kv = jnp.concatenate([k[h], v[:, h * HEAD : (h + 1) * HEAD]], axis=-1).astype(BF16)
        g = three_parts(gate[h : h + 1, :])
        lines = [g[i][:, 128 * j : 128 * (j + 1)] for i in range(3) for j in range(2)]
        lines = jnp.concatenate(lines + [jnp.zeros((10, 128), F32)], axis=0).astype(BF16)
        for s in range(8):
            msg[s, h, 0:32, :] = kv[32 * s : 32 * s + 32]
            a = q[h][32 * s : 32 * s + 16]
            b = q[h][32 * s + 16 : 32 * s + 32]
            msg[s, h, 32:48, :] = jnp.concatenate([a, b], axis=-1).astype(BF16)
            msg[s, h, 48:64, :] = lines


def attend_kernel(where, kx, ko, qy, gates, out, kv, qs, bias, gap, buf):
    y, c, s = where[0], where[1], where[2]
    lane = iota((16, 128), 1)
    for z in range(NZ):
        for x in range(NX):
            kv[pl.ds(pl.multiple_of(z * 256 + 64 * x + 32 * c, 32), 32), :] = kx[x, z]
            kv[pl.ds(pl.multiple_of(z * 256 + 64 * x + 32 - 32 * c, 32), 32), :] = ko[x, z]
        g = gates[z].astype(F32)
        g = g[0:2] + g[2:4] + g[4:6]
        for j in range(2):
            at = (z % 2) * 256 + j * 128
            bias[z // 2, :, at : at + 128] = jnp.broadcast_to(g[j : j + 1], (8, 128))
        for yy in range(NY):
            p = qy[yy, z].astype(F32)
            base = yy * 64 + (z % 2) * 32
            qs[z // 2, base : base + 16, :] = jnp.where(lane < 64, p, 0.0).astype(BF16)
            qs[z // 2, base + 16 : base + 32, :] = jnp.where(
                lane < 64, pltpu.roll(p, 64, 1), 0.0
            ).astype(BF16)
    r = iota((256, 512), 0)
    l = iota((256, 512), 1)
    q_at = (((r // 32) % 2) * 4 + r // 64) * 256 + 32 * s + r % 32
    k_at = ((l // 256) * 4 + y) * 256 + l % 256
    gap[...] = k_at - q_at

    def step(i, carry):
        low = jnp.full((256, 128), NEG, F32)
        tops = [low, low]
        for t in range(9):
            first = t <= i
            qi = jnp.where(first, i, 7 - i)
            j = jnp.where(first, t, t - i - 1)
            keys = kv[pl.ds(pl.multiple_of(j * 512, 512), 512), :]
            logits = dot_t(qs[qi], keys) - bias[j, 0:1, :]
            logits = jnp.where(gap[...] <= 2048 * (qi - j), logits, NEG)
            buf[t] = logits
            m = jnp.maximum(
                jnp.maximum(logits[:, 0:128], logits[:, 128:256]),
                jnp.maximum(logits[:, 256:384], logits[:, 384:512]),
            )
            if t == 0:
                tops[0] = m
            elif t >= 4:
                tops[1] = jnp.maximum(tops[1], m)
            else:
                tops[0] = jnp.where(first, jnp.maximum(tops[0], m), tops[0])
                tops[1] = jnp.where(first, tops[1], jnp.maximum(tops[1], m))
        tops = [jnp.maximum(jnp.max(m, axis=-1, keepdims=True), -1e29) for m in tops]
        zero = jnp.zeros((256, 128), F32)
        sums, accs = [zero, zero], [zero, zero]
        for t in range(9):
            first = t <= i
            j = jnp.where(first, t, t - i - 1)
            keys = kv[pl.ds(pl.multiple_of(j * 512, 512), 512), :]
            if t == 0:
                m = tops[0]
            elif t >= 4:
                m = tops[1]
            else:
                m = jnp.where(first, tops[0], tops[1])
            w = jnp.exp(buf[t] - m)
            n = (w[:, 0:128] + w[:, 128:256]) + (w[:, 256:384] + w[:, 384:512])
            a = dot(w.astype(BF16), keys)
            if t == 0:
                sums[0], accs[0] = n, a
            elif t >= 4:
                sums[1], accs[1] = sums[1] + n, accs[1] + a
            else:
                sums[0] = jnp.where(first, sums[0] + n, sums[0])
                accs[0] = jnp.where(first, accs[0] + a, accs[0])
                sums[1] = jnp.where(first, sums[1], sums[1] + n)
                accs[1] = jnp.where(first, accs[1], accs[1] + a)
        ln = iota((256, 128), 1)
        for k in range(2):
            n = jnp.sum(sums[k], axis=-1, keepdims=True)
            some = n > 0.0
            safe = jnp.where(some, n, 1.0)
            o = pltpu.roll(accs[k] / safe, 64, 1)
            p0, p1, p2 = three_parts(jnp.where(some, tops[k] + jnp.log(safe), NEG))
            tail = jnp.where(ln == 64, p0, jnp.where(ln == 65, p1, p2))
            o = jnp.where(ln < 64, o, jnp.where(ln < 67, tail, 0.0)).astype(BF16)
            m = i if k == 0 else 7 - i
            for yy in range(NY):
                out[yy, pl.ds(pl.multiple_of(m * 64, 64), 64), :] = o[64 * yy : 64 * yy + 64]
        return carry

    lax.fori_loop(0, 4, step, 0)


def merge_kernel(where, parts, rim, cur, out, pooled):
    x, offset = where[0], where[1]
    vals = [parts[k].astype(F32) for k in range(NY)]
    ln = iota((512, 128), 1)
    stat = (ln >= 64) & (ln < 67)
    lses = [jnp.sum(jnp.where(stat, v, 0.0), axis=-1, keepdims=True) for v in vals]
    top = jnp.maximum(jnp.maximum(lses[0], lses[1]), jnp.maximum(lses[2], lses[3]))
    ws = [jnp.exp(v - top) for v in lses]
    den = (ws[0] + ws[1]) + (ws[2] + ws[3])
    o = (ws[0] * vals[0] + ws[1] * vals[1] + ws[2] * vals[2] + ws[3] * vals[3]) / den
    o = o.reshape(16, 2, 16, 128)
    half = iota((16, 16, 128), 2) < 64
    back = pltpu.roll(o[:, 1].reshape(256, 128), 64, 1).reshape(16, 16, 128)
    out[...] = jnp.where(half, o[:, 0], back).astype(BF16)
    now = cur[...].astype(F32)
    ext = jnp.concatenate([rim[...].astype(F32), now], axis=0)
    counts = (offset + iota((ROWS, 128), 0) + 1).astype(F32)
    mean = jnp.zeros((ROWS, 128), F32)
    run = ext
    for g in range(4):
        w = 2 ** (g + 1)
        n = run.shape[0]
        run = run[w // 2 :] + run[: n - w // 2]
        avg = run[run.shape[0] - ROWS :] / jnp.minimum(counts, float(w))
        mean = jnp.where(x == g, avg, mean)
    pooled[...] = (mean - now).astype(BF16)


def output_kernel(where, own, other, wpo, wao, out, pooled, attended):
    c = where[0]
    half = iota((16, 128), 1) < 64
    for x in range(NX):
        for k, ref in enumerate((own, other)):
            s = 2 * x + (c if k == 0 else 1 - c)
            pooled[:, pl.ds(pl.multiple_of(s * 128, 128), 128)] = ref[x, 256:512, :]
            for j in range(8):
                a = ref[x, 32 * j : 32 * j + 16, :].astype(F32)
                b = ref[x, 32 * j + 16 : 32 * j + 32, :].astype(F32)
                u = jnp.where(half, a, pltpu.roll(b, 64, 1)).astype(BF16)
                v = jnp.where(half, pltpu.roll(a, 64, 1), b).astype(BF16)
                at = pl.multiple_of(s * 32, 32)
                attended[pl.ds(at, 16), 128 * j : 128 * j + 128] = u
                attended[pl.ds(at + 16, 16), 128 * j : 128 * j + 128] = v
    out[...] = (dot(pooled[...], wpo[...]) + dot(attended[...], wao[...])).astype(BF16)


VM = pl.BlockSpec(memory_space=pltpu.VMEM)
SM = pl.BlockSpec(memory_space=pltpu.SMEM)


def call(kernel, name, where, ins, outs, scratch, flops):
    shapes = [jax.ShapeDtypeStruct(s, BF16) for s in outs]
    return pl.pallas_call(
        kernel,
        name=name,
        out_shape=shapes,
        in_specs=[SM] + [VM] * len(ins),
        out_specs=[VM] * len(outs),
        scratch_shapes=scratch,
        cost_estimate=pl.CostEstimate(flops=flops, bytes_accessed=2**20, transcendentals=0),
        compiler_params=pltpu.CompilerParams(vmem_limit_bytes=48 * 2**20),
    )(jnp.stack([jnp.asarray(w, jnp.int32) for w in where]), *ins)


def swap(value):
    return lax.ppermute(value, "c", [(0, 1), (1, 0)])


def per_device(
    tokens, norm_gain, wq, wk, wv, wp, query_gain, key_gain, cum_gate, wpo, wao
):
    z, y, x, c = (lax.axis_index(a) for a in ("z", "y", "x", "c"))
    own = lax.all_gather(tokens, "x", axis=0, tiled=False)
    other = swap(own)
    msg, pool = call(
        project_kernel,
        "project",
        (c,),
        (
            own,
            other,
            norm_gain.reshape(1, 2048),
            wq,
            wk,
            wv,
            wp,
            query_gain.reshape(1, HEAD),
            key_gain.reshape(1, HEAD),
            cum_gate.T,
        ),
        [(8, 2, 64, 128), (ROWS, 128)],
        [pltpu.VMEM((ROWS, 2048), BF16)],
        2 * ROWS * 2048 * 512,
    )
    count = NZ * NY
    rim = lax.ppermute(pool[ROWS - 16 :], SP, [(k, k + 1) for k in range(count - 1)])
    heads = lax.all_to_all(msg.reshape(8, 128, 128), TP, 0, 0, tiled=True)
    mine = lax.all_to_all(heads.reshape(16, 64, 128), "z", 0, 0, tiled=True)
    kx = lax.all_gather(mine[:, 0:32], "x", axis=0, tiled=False)
    ko = swap(kx)
    qy = lax.all_gather(mine[:, 32:48], "y", axis=0, tiled=False)
    (parts,) = call(
        attend_kernel,
        "attend",
        (y, c, 2 * x + c),
        (kx, ko, qy, mine[:, 48:64]),
        [(NY, 512, 128)],
        [
            pltpu.VMEM((4096, 128), BF16),
            pltpu.VMEM((8, 256, 128), BF16),
            pltpu.VMEM((8, 8, 512), F32),
            pltpu.VMEM((256, 512), jnp.int32),
            pltpu.VMEM((9, 256, 512), F32),
        ],
        4 * 72 * 256 * 256 * 128,
    )
    parts = lax.all_to_all(parts, "y", 0, 0, tiled=True)
    merged, pooled = call(
        merge_kernel,
        "merge",
        (x, (z * NY + y) * ROWS),
        (parts, rim, pool),
        [(16, 16, 128), (ROWS, 128)],
        [],
        2**20,
    )
    back = lax.all_to_all(merged, "z", 0, 0, tiled=True)
    both = jnp.concatenate([back.reshape(256, 128), pooled], axis=0)
    own = lax.all_gather(both, "x", axis=0, tiled=False)
    other = swap(own)
    (mixed,) = call(
        output_kernel,
        "output",
        (c,),
        (own, other, wpo, wao),
        [(ROWS, 256)],
        [pltpu.VMEM((ROWS, 1024), BF16), pltpu.VMEM((ROWS, 1024), BF16)],
        2 * ROWS * 2048 * 256,
    )
    return mixed


def solution(mesh):
    grid = Mesh(mesh.devices.reshape(NZ, NY, NX, NC), ("z", "y", "x", "c"))
    return jax.shard_map(
        per_device,
        mesh=grid,
        in_specs=(
            P(SP, TP),
            P(),
            P(TP, None),
            P(TP, None),
            P(TP, None),
            P(TP, None),
            P(),
            P(),
            P(SP, TP),
            P(None, TP),
            P(None, TP),
        ),
        out_specs=P(SP, TP),
        check_vma=False,
    )
```

```python
import jax
import jax.numpy as jnp
from jax import lax
from jax.experimental import pallas as pl
from jax.experimental.pallas import tpu as pltpu
from jax.sharding import Mesh, PartitionSpec as P


F32 = jnp.float32
BF16 = jnp.bfloat16
HEAD = 64
EPS = 1e-06
NEG = -1e30
ROWS = 256
NZ, NY, NX, NC = 16, 4, 4, 2
TP = ("x", "c")
SP = ("z", "y")


def iota(shape, dim):
    return lax.broadcasted_iota(jnp.int32, shape, dim)


def dot_t(a, b):
    return lax.dot_general(a, b, (((1,), (1,)), ((), ())), preferred_element_type=F32)


def dot(a, b):
    return lax.dot_general(a, b, (((1,), (0,)), ((), ())), preferred_element_type=F32)


def three_parts(v):
    a = v.astype(BF16).astype(F32)
    b = (v - a).astype(BF16).astype(F32)
    return a, b, (v - a - b).astype(BF16).astype(F32)


def head_scale(v, gain, times):
    parts = []
    for h in range(2):
        w = v[:, h * HEAD : (h + 1) * HEAD]
        w = w * lax.rsqrt(jnp.mean(w * w, axis=-1, keepdims=True) + EPS) * gain
        parts.append(w * times if times else w)
    return parts


def project_kernel(
    where, own, other, gain, wq, wk_, wv_, wp_, qg, kg, gate, msg, pool, normed, wk, wv, wp, sems
):
    c = where[0]
    pairs = ((wk_, wk), (wv_, wv), (wp_, wp))
    copies = [pltpu.make_async_copy(a, b, sems.at[k]) for k, (a, b) in enumerate(pairs)]
    for copy in copies:
        copy.start()
    total = jnp.zeros((ROWS, 1), F32)
    for x in range(NX):
        for ref in (own, other):
            v = ref[x].astype(F32)
            total = total + jnp.sum(v * v, axis=-1, keepdims=True)
    scale = lax.rsqrt(total / 2048.0 + EPS)
    for x in range(NX):
        for k, ref in enumerate((own, other)):
            at = pl.multiple_of((2 * x + (c if k == 0 else 1 - c)) * 256, 256)
            v = ref[x].astype(F32) * scale * gain[:, pl.ds(at, 256)]
            normed[:, pl.ds(at, 256)] = v.astype(BF16)
    rows = normed[...]
    q = head_scale(dot_t(rows, wq[...]), qg[...], HEAD ** (-0.5))
    for copy in copies:
        copy.wait()
    k = head_scale(dot_t(rows, wk[...]), kg[...], None)
    v = dot_t(rows, wv[...])
    pool[...] = dot_t(rows, wp[...]).astype(BF16)
    for h in range(2):
        kv = jnp.concatenate([k[h], v[:, h * HEAD : (h + 1) * HEAD]], axis=-1).astype(BF16)
        g = three_parts(gate[h : h + 1, :])
        lines = [g[i][:, 128 * j : 128 * (j + 1)] for i in range(3) for j in range(2)]
        lines = jnp.concatenate(lines + [jnp.zeros((2, 128), F32)], axis=0).astype(BF16)
        for s in range(8):
            msg[s, h, 0:32, :] = kv[32 * s : 32 * s + 32]
            a = q[h][32 * s : 32 * s + 16]
            b = q[h][32 * s + 16 : 32 * s + 32]
            msg[s, h, 32:48, :] = jnp.concatenate([a, b], axis=-1).astype(BF16)
            msg[s, h, 48:56, :] = lines


def attend_kernel(where, ks, qy, gates, out, kv, qs, bias, gap, buf):
    y, s = where[0], where[1]
    lane = iota((16, 128), 1)
    for z in range(NZ):
        for k in range(8):
            kv[z * 256 + 32 * k : z * 256 + 32 * k + 32, :] = ks[k, z]
        g = gates[z].astype(F32)
        g = g[0:2] + g[2:4] + g[4:6]
        for j in range(2):
            at = (z % 2) * 256 + j * 128
            bias[z // 2, :, at : at + 128] = jnp.broadcast_to(g[j : j + 1], (8, 128))
        for yy in range(NY):
            p = qy[yy, z].astype(F32)
            base = yy * 64 + (z % 2) * 32
            qs[z // 2, base : base + 16, :] = jnp.where(lane < 64, p, 0.0).astype(BF16)
            qs[z // 2, base + 16 : base + 32, :] = jnp.where(
                lane < 64, pltpu.roll(p, 64, 1), 0.0
            ).astype(BF16)
    r = iota((256, 512), 0)
    l = iota((256, 512), 1)
    q_at = (((r // 32) % 2) * 4 + r // 64) * 256 + 32 * s + r % 32
    k_at = ((l // 256) * 4 + y) * 256 + l % 256
    gap[...] = k_at - q_at

    def step(i, carry):
        low = jnp.full((256, 128), NEG, F32)
        tops = [low, low]
        for t in range(9):
            first = t <= i
            qi = jnp.where(first, i, 7 - i)
            j = jnp.where(first, t, t - i - 1)
            keys = kv[pl.ds(pl.multiple_of(j * 512, 512), 512), :]
            logits = dot_t(qs[qi], keys) - bias[j, 0:1, :]
            logits = jnp.where(gap[...] <= 2048 * (qi - j), logits, NEG)
            buf[t] = logits
            m = jnp.maximum(
                jnp.maximum(logits[:, 0:128], logits[:, 128:256]),
                jnp.maximum(logits[:, 256:384], logits[:, 384:512]),
            )
            if t == 0:
                tops[0] = m
            elif t >= 4:
                tops[1] = jnp.maximum(tops[1], m)
            else:
                tops[0] = jnp.where(first, jnp.maximum(tops[0], m), tops[0])
                tops[1] = jnp.where(first, tops[1], jnp.maximum(tops[1], m))
        tops = [jnp.maximum(jnp.max(m, axis=-1, keepdims=True), -1e29) for m in tops]
        zero = jnp.zeros((256, 128), F32)
        sums, accs = [zero, zero], [zero, zero]
        for t in range(9):
            first = t <= i
            j = jnp.where(first, t, t - i - 1)
            keys = kv[pl.ds(pl.multiple_of(j * 512, 512), 512), :]
            if t == 0:
                m = tops[0]
            elif t >= 4:
                m = tops[1]
            else:
                m = jnp.where(first, tops[0], tops[1])
            w = jnp.exp(buf[t] - m)
            n = (w[:, 0:128] + w[:, 128:256]) + (w[:, 256:384] + w[:, 384:512])
            a = dot(w.astype(BF16), keys)
            if t == 0:
                sums[0], accs[0] = n, a
            elif t >= 4:
                sums[1], accs[1] = sums[1] + n, accs[1] + a
            else:
                sums[0] = jnp.where(first, sums[0] + n, sums[0])
                accs[0] = jnp.where(first, accs[0] + a, accs[0])
                sums[1] = jnp.where(first, sums[1], sums[1] + n)
                accs[1] = jnp.where(first, accs[1], accs[1] + a)
        ln = iota((256, 128), 1)
        for k in range(2):
            n = jnp.sum(sums[k], axis=-1, keepdims=True)
            some = n > 0.0
            safe = jnp.where(some, n, 1.0)
            o = pltpu.roll(accs[k] / safe, 64, 1)
            p0, p1, p2 = three_parts(jnp.where(some, tops[k] + jnp.log(safe), NEG))
            tail = jnp.where(ln == 64, p0, jnp.where(ln == 65, p1, p2))
            o = jnp.where(ln < 64, o, jnp.where(ln < 67, tail, 0.0)).astype(BF16)
            m = i if k == 0 else 7 - i
            for yy in range(NY):
                out[yy, pl.ds(pl.multiple_of(m * 64, 64), 64), :] = o[64 * yy : 64 * yy + 64]
        return carry

    lax.fori_loop(0, 4, step, 0)


def merge_kernel(where, parts, out):
    vals = [parts[k].astype(F32) for k in range(NY)]
    ln = iota((512, 128), 1)
    stat = (ln >= 64) & (ln < 67)
    lses = [jnp.sum(jnp.where(stat, v, 0.0), axis=-1, keepdims=True) for v in vals]
    top = jnp.maximum(jnp.maximum(lses[0], lses[1]), jnp.maximum(lses[2], lses[3]))
    ws = [jnp.exp(v - top) for v in lses]
    den = (ws[0] + ws[1]) + (ws[2] + ws[3])
    o = (ws[0] * vals[0] + ws[1] * vals[1] + ws[2] * vals[2] + ws[3] * vals[3]) / den
    o = o.reshape(16, 2, 16, 128)
    half = iota((16, 16, 128), 2) < 64
    back = pltpu.roll(o[:, 1].reshape(256, 128), 64, 1).reshape(16, 16, 128)
    out[...] = jnp.where(half, o[:, 0], back).astype(BF16)


def pool_kernel(where, rim, cur, pooled):
    x, offset = where[0], where[1]
    now = cur[...].astype(F32)
    ext = jnp.concatenate([rim[...].astype(F32), now], axis=0)
    counts = (offset + iota((ROWS, 128), 0) + 1).astype(F32)
    mean = jnp.zeros((ROWS, 128), F32)
    run = ext
    for g in range(4):
        w = 2 ** (g + 1)
        n = run.shape[0]
        run = run[w // 2 :] + run[: n - w // 2]
        avg = run[run.shape[0] - ROWS :] / jnp.minimum(counts, float(w))
        mean = jnp.where(x == g, avg, mean)
    pooled[...] = (mean - now).astype(BF16)


def output_kernel(where, own, other, pools, wpo, wao, out, pooled, attended):
    c = where[0]
    half = iota((16, 128), 1) < 64
    for x in range(NX):
        for k, ref in enumerate((own, other)):
            s = 2 * x + (c if k == 0 else 1 - c)
            pooled[:, 128 * (2 * x + k) : 128 * (2 * x + k + 1)] = pools[2 * x + k]
            for j in range(8):
                a = ref[x, 32 * j : 32 * j + 16, :].astype(F32)
                b = ref[x, 32 * j + 16 : 32 * j + 32, :].astype(F32)
                u = jnp.where(half, a, pltpu.roll(b, 64, 1)).astype(BF16)
                v = jnp.where(half, pltpu.roll(a, 64, 1), b).astype(BF16)
                at = pl.multiple_of(s * 32, 32)
                attended[pl.ds(at, 16), 128 * j : 128 * j + 128] = u
                attended[pl.ds(at + 16, 16), 128 * j : 128 * j + 128] = v
    out[...] = (dot(pooled[...], wpo[...]) + dot(attended[...], wao[...])).astype(BF16)


VM = pl.BlockSpec(memory_space=pltpu.VMEM)
SM = pl.BlockSpec(memory_space=pltpu.SMEM)


HB = pl.BlockSpec(memory_space=pltpu.HBM)


def call(kernel, where, ins, outs, scratch, flops, mib, in_hbm=()):
    shapes = [jax.ShapeDtypeStruct(s, BF16) for s in outs]
    return pl.pallas_call(
        kernel,
        out_shape=shapes,
        in_specs=[SM] + [HB if k in in_hbm else VM for k in range(len(ins))],
        out_specs=[VM] * len(outs),
        scratch_shapes=scratch,
        cost_estimate=pl.CostEstimate(flops=flops, bytes_accessed=2**20, transcendentals=0),
        compiler_params=pltpu.CompilerParams(vmem_limit_bytes=mib * 2**20),
    )(jnp.stack([jnp.asarray(w, jnp.int32) for w in where]), *ins)


def spread(value, axis):
    size = lax.axis_size(axis)
    copies = jnp.broadcast_to(value[None], (size, *value.shape))
    return lax.all_to_all(copies, axis, 0, 0, tiled=True)


def swap(value):
    return lax.ppermute(value, "c", [(0, 1), (1, 0)])


def layer(
    tokens, norm_gain, wq, wk, wv, wp, query_gain, key_gain, cum_gate, wpo, wao
):
    z, y, x, c = (lax.axis_index(a) for a in ("z", "y", "x", "c"))
    own = lax.all_gather(tokens, "x", axis=0, tiled=False)
    other = swap(own)
    msg, pool = call(
        project_kernel,
        (c,),
        (
            own,
            other,
            norm_gain.reshape(1, 2048),
            wq,
            wk,
            wv,
            wp,
            query_gain.reshape(1, HEAD),
            key_gain.reshape(1, HEAD),
            cum_gate.T,
        ),
        [(8, 2, 56, 128), (ROWS, 128)],
        [pltpu.VMEM((ROWS, 2048), BF16)]
        + [pltpu.VMEM((128, 2048), BF16)] * 3
        + [pltpu.SemaphoreType.DMA((3,))],
        2 * ROWS * 2048 * 512,
        52,
        (4, 5, 6),
    )
    count = NZ * NY
    rim = lax.ppermute(pool[ROWS - 16 :], SP, [(k, k + 1) for k in range(count - 1)])
    heads = lax.all_to_all(msg.reshape(8, 112, 128), TP, 0, 0, tiled=True)
    mine = lax.all_to_all(heads.reshape(16, 56, 128), "z", 0, 0, tiled=True)
    ks = spread(mine[:, 0:32], TP)
    qy = lax.all_gather(mine[:, 32:48], "y", axis=0, tiled=False)
    (pooled,) = call(
        pool_kernel, (x, (z * NY + y) * ROWS), (rim, pool), [(ROWS, 128)], [], 2**20, 4
    )
    pools = spread(pooled, TP)
    (parts,) = call(
        attend_kernel,
        (y, 2 * x + c),
        (ks, qy, mine[:, 48:56]),
        [(NY, 512, 128)],
        [
            pltpu.VMEM((4096, 128), BF16),
            pltpu.VMEM((8, 256, 128), BF16),
            pltpu.VMEM((8, 8, 512), F32),
            pltpu.VMEM((256, 512), jnp.int32),
            pltpu.VMEM((9, 256, 512), F32),
        ],
        4 * 72 * 256 * 256 * 128,
        24,
    )
    parts, pools = lax.optimization_barrier((parts, pools))
    parts = lax.all_to_all(parts, "y", 0, 0, tiled=True)
    (merged,) = call(merge_kernel, (c,), (parts,), [(16, 16, 128)], [], 2**20, 8)
    back = lax.all_to_all(merged, "z", 0, 0, tiled=True)
    own = lax.all_gather(back.reshape(256, 128), "x", axis=0, tiled=False)
    other = swap(own)
    (mixed,) = call(
        output_kernel,
        (c,),
        (own, other, pools, wpo, wao),
        [(ROWS, 256)],
        [pltpu.VMEM((ROWS, 1024), BF16), pltpu.VMEM((ROWS, 1024), BF16)],
        2 * ROWS * 2048 * 256,
        12,
    )
    return mixed


def solution(mesh):
    grid = Mesh(mesh.devices.reshape(NZ, NY, NX, NC), ("z", "y", "x", "c"))
    return jax.shard_map(
        layer,
        mesh=grid,
        in_specs=(
            P(SP, TP),
            P(),
            P(TP, None),
            P(TP, None),
            P(TP, None),
            P(TP, None),
            P(),
            P(),
            P(SP, TP),
            P(None, TP),
            P(None, TP),
        ),
        out_specs=P(SP, TP),
        check_vma=False,
    )
```

```python
import jax
import jax.numpy as jnp
from jax import lax
from jax.experimental import pallas as pl
from jax.experimental.pallas import tpu as pltpu
from jax.sharding import Mesh, PartitionSpec as P


F32 = jnp.float32
BF16 = jnp.bfloat16
HEAD = 64
EPS = 1e-06
NEG = -1e30
ROWS = 256
NZ, NY, NX, NC = 16, 4, 4, 2
TP = ("x", "c")
SP = ("z", "y")


def iota(shape, dim):
    return lax.broadcasted_iota(jnp.int32, shape, dim)


def dot_t(a, b):
    return lax.dot_general(a, b, (((1,), (1,)), ((), ())), preferred_element_type=F32)


def dot(a, b):
    return lax.dot_general(a, b, (((1,), (0,)), ((), ())), preferred_element_type=F32)


def three_parts(v):
    a = v.astype(BF16).astype(F32)
    b = (v - a).astype(BF16).astype(F32)
    return a, b, (v - a - b).astype(BF16).astype(F32)


def head_scale(v, gain, times):
    parts = []
    for h in range(2):
        w = v[:, h * HEAD : (h + 1) * HEAD]
        w = w * lax.rsqrt(jnp.mean(w * w, axis=-1, keepdims=True) + EPS) * gain
        parts.append(w * times if times else w)
    return parts


def project_kernel(
    where, own, other, gain, wq, wk_, wv_, wp_, qg, kg, gate, msg, pool, normed, wk, wv, wp, sems
):
    c = where[0]
    pairs = ((wk_, wk), (wv_, wv), (wp_, wp))
    copies = [pltpu.make_async_copy(a, b, sems.at[k]) for k, (a, b) in enumerate(pairs)]
    for copy in copies:
        copy.start()
    total = jnp.zeros((ROWS, 1), F32)
    for x in range(NX):
        for ref in (own, other):
            v = ref[x].astype(F32)
            total = total + jnp.sum(v * v, axis=-1, keepdims=True)
    scale = lax.rsqrt(total / 2048.0 + EPS)
    for x in range(NX):
        for k, ref in enumerate((own, other)):
            at = pl.multiple_of((2 * x + (c if k == 0 else 1 - c)) * 256, 256)
            v = ref[x].astype(F32) * scale * gain[:, pl.ds(at, 256)]
            normed[:, pl.ds(at, 256)] = v.astype(BF16)
    rows = normed[...]
    q = head_scale(dot_t(rows, wq[...]), qg[...], HEAD ** (-0.5))
    for copy in copies:
        copy.wait()
    k = head_scale(dot_t(rows, wk[...]), kg[...], None)
    v = dot_t(rows, wv[...])
    pool[...] = dot_t(rows, wp[...]).astype(BF16)
    for h in range(2):
        kv = jnp.concatenate([k[h], v[:, h * HEAD : (h + 1) * HEAD]], axis=-1).astype(BF16)
        g = three_parts(gate[h : h + 1, :])
        zero = jnp.zeros((1, 128), F32)
        lines = []
        for j in range(2):
            lines += [v[:, 128 * j : 128 * (j + 1)] for v in g] + [zero]
        lines = jnp.concatenate(lines, axis=0).astype(BF16)
        for s in range(8):
            msg[s, h, 0:32, :] = kv[32 * s : 32 * s + 32]
            a = q[h][32 * s : 32 * s + 16]
            b = q[h][32 * s + 16 : 32 * s + 32]
            msg[s, h, 32:48, :] = jnp.concatenate([a, b], axis=-1).astype(BF16)
            msg[s, h, 48:56, :] = lines


def attend_kernel(where, ks, qy, gates, out, kv, vt, qs, gap, buf, lse):
    y, s = where[0], where[1]
    lane = iota((16, 128), 1)
    for z in range(NZ):
        for k in range(8):
            kv[z * 256 + 32 * k : z * 256 + 32 * k + 32, 0:128] = ks[k, z]
        g = gates[z].astype(F32).T
        pad = jnp.zeros((128, 120), F32)
        for j in range(2):
            part = jnp.where(iota((128, 8), 1) // 4 == j, g, 0.0)
            at = z * 256 + 128 * j
            kv[at : at + 128, 128:256] = jnp.concatenate([part, pad], axis=1).astype(BF16)
            vt[:, at : at + 128] = kv[at : at + 128, 0:128].T[64:128]
        for yy in range(NY):
            p = qy[yy, z].astype(F32)
            for half in range(2):
                base = half * 128 + yy * 32 + (z % 2) * 16
                q = p if half == 0 else pltpu.roll(p, 64, 1)
                qs[z // 2, base : base + 16, 0:128] = jnp.where(lane < 64, q, 0.0).astype(BF16)
    ln = iota((256, 128), 1)
    signs = jnp.where((ln < 7) & (ln != 3), -1.0, 0.0).astype(BF16)
    for m in range(8):
        qs[m, :, 128:256] = signs
    r = iota((512, 256), 0)
    l = iota((512, 256), 1)
    k_at = ((r // 256) * 4 + y) * 256 + r % 256
    q_at = (((l // 16) % 2) * 4 + (l // 32) % 4) * 256 + 32 * s + (l // 128) * 16 + l % 16
    gap[...] = k_at - q_at

    def step(i, carry):
        low = jnp.full((8, 256), NEG, F32)
        tops = [low, low]
        for t in range(9):
            first = t <= i
            qi = jnp.where(first, i, 7 - i)
            j = jnp.where(first, t, t - i - 1)
            keys = kv[pl.ds(pl.multiple_of(j * 512, 512), 512), :]
            logits = dot_t(keys, qs[qi])
            logits = jnp.where(gap[...] <= 2048 * (qi - j), logits, NEG)
            buf[t] = logits
            m = jnp.max(logits.reshape(64, 8, 256), axis=0)
            if t == 0:
                tops[0] = m
            elif t >= 4:
                tops[1] = jnp.maximum(tops[1], m)
            else:
                tops[0] = jnp.where(first, jnp.maximum(tops[0], m), tops[0])
                tops[1] = jnp.where(first, tops[1], jnp.maximum(tops[1], m))
        tops = [jnp.maximum(jnp.max(m, axis=0, keepdims=True), -1e29) for m in tops]
        sums = [jnp.zeros((8, 256), F32)] * 2
        accs = [jnp.zeros((64, 256), F32)] * 2
        for t in range(9):
            first = t <= i
            j = jnp.where(first, t, t - i - 1)
            if t == 0:
                m = tops[0]
            elif t >= 4:
                m = tops[1]
            else:
                m = jnp.where(first, tops[0], tops[1])
            w = jnp.exp(buf[t] - m)
            n = jnp.sum(w.reshape(64, 8, 256), axis=0)
            a = dot(vt[:, pl.ds(pl.multiple_of(j * 512, 512), 512)], w.astype(BF16))
            if t == 0:
                sums[0], accs[0] = n, a
            elif t >= 4:
                sums[1], accs[1] = sums[1] + n, accs[1] + a
            else:
                sums[0] = jnp.where(first, sums[0] + n, sums[0])
                accs[0] = jnp.where(first, accs[0] + a, accs[0])
                sums[1] = jnp.where(first, sums[1], sums[1] + n)
                accs[1] = jnp.where(first, accs[1], accs[1] + a)
        for k in range(2):
            n = jnp.sum(sums[k], axis=0, keepdims=True)
            some = n > 0.0
            safe = jnp.where(some, n, 1.0)
            m = i if k == 0 else 7 - i
            lse[pl.ds(m, 1), :] = jnp.where(some, tops[k] + jnp.log(safe), NEG)
            o = accs[k] / safe
            o = jnp.concatenate([o[:, 0:128], o[:, 128:256]], axis=0).T.astype(BF16)
            for yy in range(NY):
                at = pl.multiple_of(m * 32, 32)
                out[yy, pl.ds(at, 32), :] = o[32 * yy : 32 * yy + 32]
        return carry

    lax.fori_loop(0, 4, step, 0)
    ln = iota((8, 128), 1)
    for yy in range(NY):
        a = pltpu.roll(lse[:, 0:128], (128 - 32 * yy) % 128, 1)
        b = pltpu.roll(lse[:, 128:256], (160 - 32 * yy) % 128, 1)
        v = jnp.where(ln < 32, a, jnp.where(ln < 64, b, 0.0))
        out[yy, 256:280, :] = jnp.concatenate(three_parts(v), axis=0).astype(BF16)


def merge_kernel(where, parts, out):
    lses = []
    for k in range(NY):
        v = parts[k, 256:280, :].astype(F32)
        lses.append(v[0:8] + v[8:16] + v[16:24])
    top = jnp.maximum(jnp.maximum(lses[0], lses[1]), jnp.maximum(lses[2], lses[3]))
    ws = [jnp.exp(v - top) for v in lses]
    den = (ws[0] + ws[1]) + (ws[2] + ws[3])
    ws = [(w / den).T for w in ws]
    half = iota((16, 128), 1) < 64
    for z in range(NZ):
        m, at = z // 2, (z % 2) * 16
        total = jnp.zeros((16, 128), F32)
        for k in range(NY):
            a = ws[k][at : at + 16, m : m + 1]
            b = ws[k][at + 32 : at + 48, m : m + 1]
            total = total + jnp.where(half, a, b) * parts[k, 16 * z : 16 * z + 16, :].astype(F32)
        out[z] = total.astype(BF16)


def pool_kernel(where, rim, cur, pooled):
    x, offset = where[0], where[1]
    now = cur[...].astype(F32)
    ext = jnp.concatenate([rim[...].astype(F32), now], axis=0)
    counts = (offset + iota((ROWS, 128), 0) + 1).astype(F32)
    mean = jnp.zeros((ROWS, 128), F32)
    run = ext
    for g in range(4):
        w = 2 ** (g + 1)
        n = run.shape[0]
        run = run[w // 2 :] + run[: n - w // 2]
        avg = run[run.shape[0] - ROWS :] / jnp.minimum(counts, float(w))
        mean = jnp.where(x == g, avg, mean)
    pooled[...] = (mean - now).astype(BF16)


def output_kernel(where, own, other, wpo, wao, out, pooled, attended):
    c = where[0]
    half = iota((16, 128), 1) < 64
    for x in range(NX):
        for k, ref in enumerate((own, other)):
            s = 2 * x + (c if k == 0 else 1 - c)
            pooled[:, pl.ds(pl.multiple_of(s * 128, 128), 128)] = ref[x, 256:512, :]
            for j in range(8):
                a = ref[x, 32 * j : 32 * j + 16, :].astype(F32)
                b = ref[x, 32 * j + 16 : 32 * j + 32, :].astype(F32)
                u = jnp.where(half, a, pltpu.roll(b, 64, 1)).astype(BF16)
                v = jnp.where(half, pltpu.roll(a, 64, 1), b).astype(BF16)
                at = pl.multiple_of(s * 32, 32)
                attended[pl.ds(at, 16), 128 * j : 128 * j + 128] = u
                attended[pl.ds(at + 16, 16), 128 * j : 128 * j + 128] = v
    out[...] = (dot(pooled[...], wpo[...]) + dot(attended[...], wao[...])).astype(BF16)


VM = pl.BlockSpec(memory_space=pltpu.VMEM)
SM = pl.BlockSpec(memory_space=pltpu.SMEM)


HB = pl.BlockSpec(memory_space=pltpu.HBM)


def call(kernel, where, ins, outs, scratch, flops, mib, in_hbm=()):
    shapes = [jax.ShapeDtypeStruct(s, BF16) for s in outs]
    return pl.pallas_call(
        kernel,
        out_shape=shapes,
        in_specs=[SM] + [HB if k in in_hbm else VM for k in range(len(ins))],
        out_specs=[VM] * len(outs),
        scratch_shapes=scratch,
        cost_estimate=pl.CostEstimate(flops=flops, bytes_accessed=2**20, transcendentals=0),
        compiler_params=pltpu.CompilerParams(vmem_limit_bytes=mib * 2**20),
    )(jnp.stack([jnp.asarray(w, jnp.int32) for w in where]), *ins)


def spread(value, axis):
    size = lax.axis_size(axis)
    copies = jnp.broadcast_to(value[None], (size, *value.shape))
    return lax.all_to_all(copies, axis, 0, 0, tiled=True)


def swap(value):
    return lax.ppermute(value, "c", [(0, 1), (1, 0)])


def layer(
    tokens, norm_gain, wq, wk, wv, wp, query_gain, key_gain, cum_gate, wpo, wao
):
    z, y, x, c = (lax.axis_index(a) for a in ("z", "y", "x", "c"))
    own = lax.all_gather(tokens, "x", axis=0, tiled=False)
    other = swap(own)
    msg, pool = call(
        project_kernel,
        (c,),
        (
            own,
            other,
            norm_gain.reshape(1, 2048),
            wq,
            wk,
            wv,
            wp,
            query_gain.reshape(1, HEAD),
            key_gain.reshape(1, HEAD),
            cum_gate.T,
        ),
        [(8, 2, 56, 128), (ROWS, 128)],
        [pltpu.VMEM((ROWS, 2048), BF16)]
        + [pltpu.VMEM((128, 2048), BF16)] * 3
        + [pltpu.SemaphoreType.DMA((3,))],
        2 * ROWS * 2048 * 512,
        52,
        (4, 5, 6),
    )
    count = NZ * NY
    heads = lax.all_to_all(msg.reshape(8, 112, 128), TP, 0, 0, tiled=True)
    mine = lax.all_to_all(heads.reshape(16, 56, 128), "z", 0, 0, tiled=True)
    ks = spread(mine[:, 0:32], TP)
    qy = lax.all_gather(mine[:, 32:48], "y", axis=0, tiled=False)
    (parts,) = call(
        attend_kernel,
        (y, 2 * x + c),
        (ks, qy, mine[:, 48:56]),
        [(NY, 280, 128)],
        [
            pltpu.VMEM((4096, 256), BF16),
            pltpu.VMEM((64, 4096), BF16),
            pltpu.VMEM((8, 256, 256), BF16),
            pltpu.VMEM((512, 256), jnp.int32),
            pltpu.VMEM((9, 512, 256), F32),
            pltpu.VMEM((8, 256), F32),
        ],
        4 * 72 * 256 * 256 * 128,
        24,
    )
    parts = lax.all_to_all(parts, "y", 0, 0, tiled=True)
    (merged,) = call(merge_kernel, (c,), (parts,), [(16, 16, 128)], [], 2**20, 8)
    rim = lax.ppermute(pool[ROWS - 16 :], SP, [(k, k + 1) for k in range(count - 1)])
    (pooled,) = call(
        pool_kernel, (x, (z * NY + y) * ROWS), (rim, pool), [(ROWS, 128)], [], 2**20, 4
    )
    back = lax.all_to_all(merged, "z", 0, 0, tiled=True)
    both = jnp.concatenate([back.reshape(256, 128), pooled], axis=0)
    own = lax.all_gather(both, "x", axis=0, tiled=False)
    other = swap(own)
    (mixed,) = call(
        output_kernel,
        (c,),
        (own, other, wpo, wao),
        [(ROWS, 256)],
        [pltpu.VMEM((ROWS, 1024), BF16), pltpu.VMEM((ROWS, 1024), BF16)],
        2 * ROWS * 2048 * 256,
        12,
    )
    return mixed


def solution(mesh):
    grid = Mesh(mesh.devices.reshape(NZ, NY, NX, NC), ("z", "y", "x", "c"))
    return jax.shard_map(
        layer,
        mesh=grid,
        in_specs=(
            P(SP, TP),
            P(),
            P(TP, None),
            P(TP, None),
            P(TP, None),
            P(TP, None),
            P(),
            P(),
            P(SP, TP),
            P(None, TP),
            P(None, TP),
        ),
        out_specs=P(SP, TP),
        check_vma=False,
    )
```

```python
import jax
import jax.numpy as jnp
from jax import lax
from jax.experimental import pallas as pl
from jax.experimental.pallas import tpu as pltpu
from jax.sharding import Mesh, PartitionSpec as P


F32 = jnp.float32
BF16 = jnp.bfloat16
HEAD = 64
EPS = 1e-06
NEG = -1e30
ROWS = 256
NZ, NY, NX, NC = 16, 4, 4, 2
TP = ("x", "c")
SP = ("z", "y")


def iota(shape, dim):
    return lax.broadcasted_iota(jnp.int32, shape, dim)


def dot_t(a, b):
    return lax.dot_general(a, b, (((1,), (1,)), ((), ())), preferred_element_type=F32)


def dot(a, b):
    return lax.dot_general(a, b, (((1,), (0,)), ((), ())), preferred_element_type=F32)


def three_parts(v):
    a = v.astype(BF16).astype(F32)
    b = (v - a).astype(BF16).astype(F32)
    return a, b, (v - a - b).astype(BF16).astype(F32)


def head_scale(v, gain, times):
    parts = []
    for h in range(2):
        w = v[:, h * HEAD : (h + 1) * HEAD]
        w = w * lax.rsqrt(jnp.mean(w * w, axis=-1, keepdims=True) + EPS) * gain
        parts.append(w * times if times else w)
    return parts


def project_kernel(
    where, own, other, gain, wq, wk_, wv_, wp_, qg, kg, gate, msg, pool, normed, wk, wv, wp, sems
):
    c = where[0]
    pairs = ((wk_, wk), (wv_, wv), (wp_, wp))
    copies = []
    for k, (a, b) in enumerate(pairs):
        for j in range(4):
            part = pl.ds(32 * j, 32)
            copies.append(pltpu.make_async_copy(a.at[part], b.at[part], sems.at[4 * k + j]))
    for copy in copies:
        copy.start()
    total = jnp.zeros((ROWS, 1), F32)
    for x in range(NX):
        for ref in (own, other):
            v = ref[x].astype(F32)
            total = total + jnp.sum(v * v, axis=-1, keepdims=True)
    scale = lax.rsqrt(total / 2048.0 + EPS)
    for x in range(NX):
        for k, ref in enumerate((own, other)):
            at = pl.multiple_of((2 * x + (c if k == 0 else 1 - c)) * 256, 256)
            v = ref[x].astype(F32) * scale * gain[:, pl.ds(at, 256)]
            normed[:, pl.ds(at, 256)] = v.astype(BF16)
    rows = normed[...]
    q = head_scale(dot_t(rows, wq[...]), qg[...], HEAD ** (-0.5))
    for copy in copies[0:4]:
        copy.wait()
    k = head_scale(dot_t(rows, wk[...]), kg[...], None)
    for copy in copies[4:8]:
        copy.wait()
    v = dot_t(rows, wv[...])
    for copy in copies[8:12]:
        copy.wait()
    pool[...] = dot_t(rows, wp[...]).astype(BF16)
    for h in range(2):
        kv = jnp.concatenate([k[h], v[:, h * HEAD : (h + 1) * HEAD]], axis=-1).astype(BF16)
        g = three_parts(gate[h : h + 1, :])
        zero = jnp.zeros((1, 128), F32)
        lines = []
        for j in range(2):
            lines += [v[:, 128 * j : 128 * (j + 1)] for v in g] + [zero]
        lines = jnp.concatenate(lines, axis=0).astype(BF16)
        for s in range(8):
            msg[s, h, 0:32, :] = kv[32 * s : 32 * s + 32]
            a = q[h][32 * s : 32 * s + 16]
            b = q[h][32 * s + 16 : 32 * s + 32]
            msg[s, h, 32:48, :] = jnp.concatenate([a, b], axis=-1).astype(BF16)
            msg[s, h, 48:56, :] = lines


def place(i, t):
    if t <= i:
        return i, (i, *range(i))[t], 0
    return 7 - i, t - i - 1, 1


def prepare_kernel(where, qy, gates, qs, side, mask):
    y, s = where[0], where[1]
    lane = iota((16, 128), 1)
    for z in range(NZ):
        for yy in range(NY):
            p = qy[yy, z].astype(F32)
            for half in range(2):
                base = half * 128 + yy * 32 + (z % 2) * 16
                q = p if half == 0 else pltpu.roll(p, 64, 1)
                qs[z // 2, base : base + 16, 0:128] = jnp.where(lane < 64, q, 0.0).astype(BF16)
    side[...] = gates[...].astype(F32).reshape(128, 128).T
    for m in range(8):
        qs[m, :, 128:256] = jnp.full((256, 128), -1.0, BF16)
    r = iota((512, 256), 0)
    l = iota((512, 256), 1)
    k_at = ((r // 256) * 4 + y) * 256 + r % 256
    q_at = (((l // 16) % 2) * 4 + (l // 32) % 4) * 256 + 32 * s + (l // 128) * 16 + l % 16
    mask[...] = jnp.where(k_at <= q_at, 0.0, NEG)


def attend_kernel(ks, qs, side, mask, out, kv, vt, buf_a, buf_b, lse):
    for z in range(NZ):
        for k in range(8):
            kv[z * 256 + 32 * k : z * 256 + 32 * k + 32, 0:128] = ks[k, z]
        for j in range(2):
            at = z * 256 + 128 * j
            mine = iota((128, 128), 1) // 4 == 2 * z + j
            kv[at : at + 128, 128:256] = jnp.where(mine, side[...], 0.0).astype(BF16)
            vt[:, at : at + 128] = kv[at : at + 128, 0:128].T[64:128]

    def logits_of(i, buf):
        tops = [None, None]
        for t in range(9):
            qi, j, k = place(i, t)
            v = dot_t(kv[512 * j : 512 * j + 512, :], qs[qi])
            if qi == j:
                v = v + mask[...]
            buf[t] = v
            m = jnp.max(v.reshape(64, 8, 256), axis=0)
            tops[k] = m if tops[k] is None else jnp.maximum(tops[k], m)
        return [jnp.maximum(jnp.max(m, axis=0, keepdims=True), -1e29) for m in tops]

    def weigh(i, buf, tops):
        sums, accs = [0.0, 0.0], [0.0, 0.0]
        for t in range(9):
            _, j, k = place(i, t)
            w = jnp.exp(buf[t] - tops[k])
            sums[k] = sums[k] + jnp.sum(w.reshape(64, 8, 256), axis=0)
            accs[k] = accs[k] + dot(vt[:, 512 * j : 512 * j + 512], w.astype(BF16))
        for k, m in ((0, i), (1, 7 - i)):
            n = jnp.sum(sums[k], axis=0, keepdims=True)
            some = n > 0.0
            safe = jnp.where(some, n, 1.0)
            lse[m : m + 1, :] = jnp.where(some, tops[k] + jnp.log(safe), NEG)
            o = accs[k] / safe
            o = jnp.concatenate([o[:, 0:128], o[:, 128:256]], axis=0).T.astype(BF16)
            for yy in range(NY):
                out[yy, 32 * m : 32 * m + 32, :] = o[32 * yy : 32 * yy + 32]

    bufs = (buf_a, buf_b)
    tops = logits_of(0, buf_a)
    for i in range(4):
        if i < 3:
            later = logits_of(i + 1, bufs[(i + 1) % 2])
        weigh(i, bufs[i % 2], tops)
        tops = later
    ln = iota((8, 128), 1)
    for yy in range(NY):
        a = pltpu.roll(lse[:, 0:128], (128 - 32 * yy) % 128, 1)
        b = pltpu.roll(lse[:, 128:256], (160 - 32 * yy) % 128, 1)
        v = jnp.where(ln < 32, a, jnp.where(ln < 64, b, 0.0))
        out[yy, 256:280, :] = jnp.concatenate(three_parts(v), axis=0).astype(BF16)


def merge_kernel(parts, out):
    lses = []
    for k in range(NY):
        v = parts[k, 256:280, :].astype(F32)
        lses.append(v[0:8] + v[8:16] + v[16:24])
    top = jnp.maximum(jnp.maximum(lses[0], lses[1]), jnp.maximum(lses[2], lses[3]))
    ws = [jnp.exp(v - top) for v in lses]
    den = (ws[0] + ws[1]) + (ws[2] + ws[3])
    ws = [(w / den).T for w in ws]
    half = iota((16, 128), 1) < 64
    for z in range(NZ):
        m, at = z // 2, (z % 2) * 16
        total = jnp.zeros((16, 128), F32)
        for k in range(NY):
            a = ws[k][at : at + 16, m : m + 1]
            b = ws[k][at + 32 : at + 48, m : m + 1]
            total = total + jnp.where(half, a, b) * parts[k, 16 * z : 16 * z + 16, :].astype(F32)
        out[z] = total.astype(BF16)


def pool_kernel(where, rim, cur, pooled):
    x, offset = where[0], where[1]
    now = cur[...].astype(F32)
    ext = jnp.concatenate([rim[...].astype(F32), now], axis=0)
    counts = (offset + iota((ROWS, 128), 0) + 1).astype(F32)
    mean = jnp.zeros((ROWS, 128), F32)
    run = ext
    for g in range(4):
        w = 2 ** (g + 1)
        n = run.shape[0]
        run = run[w // 2 :] + run[: n - w // 2]
        avg = run[run.shape[0] - ROWS :] / jnp.minimum(counts, float(w))
        mean = jnp.where(x == g, avg, mean)
    pooled[...] = (mean - now).astype(BF16)


def output_kernel(where, own, other, wpo, wao, out, pooled, attended):
    c = where[0]
    half = iota((16, 128), 1) < 64
    for x in range(NX):
        for k, ref in enumerate((own, other)):
            s = 2 * x + (c if k == 0 else 1 - c)
            pooled[:, pl.ds(pl.multiple_of(s * 128, 128), 128)] = ref[x, 256:512, :]
            for j in range(8):
                a = ref[x, 32 * j : 32 * j + 16, :].astype(F32)
                b = ref[x, 32 * j + 16 : 32 * j + 32, :].astype(F32)
                u = jnp.where(half, a, pltpu.roll(b, 64, 1)).astype(BF16)
                v = jnp.where(half, pltpu.roll(a, 64, 1), b).astype(BF16)
                at = pl.multiple_of(s * 32, 32)
                attended[pl.ds(at, 16), 128 * j : 128 * j + 128] = u
                attended[pl.ds(at + 16, 16), 128 * j : 128 * j + 128] = v
    out[...] = (dot(pooled[...], wpo[...]) + dot(attended[...], wao[...])).astype(BF16)


VM = pl.BlockSpec(memory_space=pltpu.VMEM)
SM = pl.BlockSpec(memory_space=pltpu.SMEM)


HB = pl.BlockSpec(memory_space=pltpu.HBM)


def call(kernel, where, ins, outs, scratch, flops, mib, in_hbm=()):
    head = [jnp.stack([jnp.asarray(w, jnp.int32) for w in where])] if where else []
    shapes = [jax.ShapeDtypeStruct(s, F32 if s in ((512, 256), (128, 128)) else BF16) for s in outs]
    return pl.pallas_call(
        kernel,
        out_shape=shapes,
        in_specs=[SM] * len(head) + [HB if k in in_hbm else VM for k in range(len(ins))],
        out_specs=[VM] * len(outs),
        scratch_shapes=scratch,
        cost_estimate=pl.CostEstimate(flops=flops, bytes_accessed=2**20, transcendentals=0),
        compiler_params=pltpu.CompilerParams(vmem_limit_bytes=mib * 2**20),
    )(*head, *ins)


def spread(value, axis):
    size = lax.axis_size(axis)
    copies = jnp.broadcast_to(value[None], (size, *value.shape))
    return lax.all_to_all(copies, axis, 0, 0, tiled=True)


def swap(value):
    return lax.ppermute(value, "c", [(0, 1), (1, 0)])


def layer(
    tokens, norm_gain, wq, wk, wv, wp, query_gain, key_gain, cum_gate, wpo, wao
):
    z, y, x, c = (lax.axis_index(a) for a in ("z", "y", "x", "c"))
    own = lax.all_gather(tokens, "x", axis=0, tiled=False)
    other = swap(own)
    msg, pool = call(
        project_kernel,
        (c,),
        (
            own,
            other,
            norm_gain.reshape(1, 2048),
            wq,
            wk,
            wv,
            wp,
            query_gain.reshape(1, HEAD),
            key_gain.reshape(1, HEAD),
            cum_gate.T,
        ),
        [(8, 2, 56, 128), (ROWS, 128)],
        [pltpu.VMEM((ROWS, 2048), BF16)]
        + [pltpu.VMEM((128, 2048), BF16)] * 3
        + [pltpu.SemaphoreType.DMA((12,))],
        2 * ROWS * 2048 * 512,
        52,
        (4, 5, 6),
    )
    count = NZ * NY
    heads = lax.all_to_all(msg.reshape(8, 112, 128), TP, 0, 0, tiled=True)
    mine = lax.all_to_all(heads.reshape(16, 56, 128), "z", 0, 0, tiled=True)
    ks = spread(mine[:, 0:32], TP)
    qy = lax.all_gather(mine[:, 32:48], "y", axis=0, tiled=False)
    qs, side, mask = call(
        prepare_kernel,
        (y, 2 * x + c),
        (qy, mine[:, 48:56]),
        [(8, 256, 256), (128, 128), (512, 256)],
        [],
        2**20,
        8,
    )
    (parts,) = call(
        attend_kernel,
        (),
        (ks, qs, side, mask),
        [(NY, 280, 128)],
        [
            pltpu.VMEM((4096, 256), BF16),
            pltpu.VMEM((64, 4096), BF16),
            pltpu.VMEM((9, 512, 256), F32),
            pltpu.VMEM((9, 512, 256), F32),
            pltpu.VMEM((8, 256), F32),
        ],
        4 * 72 * 256 * 256 * 128,
        28,
    )
    parts = lax.all_to_all(parts, "y", 0, 0, tiled=True)
    (merged,) = call(merge_kernel, (), (parts,), [(16, 16, 128)], [], 2**20, 8)
    rim = lax.ppermute(pool[ROWS - 16 :], SP, [(k, k + 1) for k in range(count - 1)])
    (pooled,) = call(
        pool_kernel, (x, (z * NY + y) * ROWS), (rim, pool), [(ROWS, 128)], [], 2**20, 4
    )
    back = lax.all_to_all(merged, "z", 0, 0, tiled=True)
    both = jnp.concatenate([back.reshape(256, 128), pooled], axis=0)
    own = lax.all_gather(both, "x", axis=0, tiled=False)
    other = swap(own)
    (mixed,) = call(
        output_kernel,
        (c,),
        (own, other, wpo, wao),
        [(ROWS, 256)],
        [pltpu.VMEM((ROWS, 1024), BF16), pltpu.VMEM((ROWS, 1024), BF16)],
        2 * ROWS * 2048 * 256,
        12,
    )
    return mixed


def solution(mesh):
    grid = Mesh(mesh.devices.reshape(NZ, NY, NX, NC), ("z", "y", "x", "c"))
    return jax.shard_map(
        layer,
        mesh=grid,
        in_specs=(
            P(SP, TP),
            P(),
            P(TP, None),
            P(TP, None),
            P(TP, None),
            P(TP, None),
            P(),
            P(),
            P(SP, TP),
            P(None, TP),
            P(None, TP),
        ),
        out_specs=P(SP, TP),
        check_vma=False,
    )
```

```python
import jax
import jax.numpy as jnp
from jax import lax
from jax.experimental import pallas as pl
from jax.experimental.pallas import tpu as pltpu
from jax.sharding import Mesh, PartitionSpec as P


F32 = jnp.float32
BF16 = jnp.bfloat16
HEAD = 64
EPS = 1e-06
NEG = -1e30
ROWS = 256
SUB = 32
NZ, NY, NX, NC = 16, 4, 4, 2
TP = ("x", "c")
SP = ("z", "y")


def iota(shape, dim):
    return lax.broadcasted_iota(jnp.int32, shape, dim)


def dot_t(a, b):
    return lax.dot_general(a, b, (((1,), (1,)), ((), ())), preferred_element_type=F32)


def dot(a, b):
    return lax.dot_general(a, b, (((1,), (0,)), ((), ())), preferred_element_type=F32)


def three_parts(v):
    a = v.astype(BF16).astype(F32)
    b = (v - a).astype(BF16).astype(F32)
    return a, b, (v - a - b).astype(BF16).astype(F32)


def head_scale(v, gain, times):
    parts = []
    for h in range(2):
        w = v[:, h * HEAD : (h + 1) * HEAD]
        w = w * lax.rsqrt(jnp.mean(w * w, axis=-1, keepdims=True) + EPS) * gain
        parts.append(w * times if times else w)
    return parts


def early_kernel(own, squares):
    total = jnp.zeros((ROWS, 128), F32)
    for x in range(NX):
        v = own[x].astype(F32)
        total = total + v[:, 0:128] * v[:, 0:128] + v[:, 128:256] * v[:, 128:256]
    squares[...] = total


def project_kernel(
    where, own, other, squares, gain, wq, wk, wv_, wp_, qg, kg, gate, msg, pool, normed, wv, wp, sems
):
    c = where[0]
    copies = []
    for k, (a, b) in enumerate(((wv_, wv), (wp_, wp))):
        copies.append(pltpu.make_async_copy(a, b, sems.at[k]))
        copies[k].start(priority=k)
    total = squares[...]
    for x in range(NX):
        v = other[x].astype(F32)
        total = total + v[:, 0:128] * v[:, 0:128] + v[:, 128:256] * v[:, 128:256]
    scale = lax.rsqrt(jnp.sum(total, axis=-1, keepdims=True) / 2048.0 + EPS)
    for x in range(NX):
        for k, ref in enumerate((own, other)):
            at = pl.multiple_of((2 * x + (c if k == 0 else 1 - c)) * 256, 256)
            v = ref[x].astype(F32) * scale * gain[:, pl.ds(at, 256)]
            normed[:, pl.ds(at, 256)] = v.astype(BF16)
    rows = normed[...]
    q = head_scale(dot_t(rows, wq[...]), qg[...], HEAD ** (-0.5))
    k = head_scale(dot_t(rows, wk[...]), kg[...], None)
    copies[0].wait()
    v = dot_t(rows, wv[...])
    for h in range(2):
        kv = jnp.concatenate([k[h], v[:, h * HEAD : (h + 1) * HEAD]], axis=-1).astype(BF16)
        g = three_parts(gate[h : h + 1, :])
        zero = jnp.zeros((1, 128), F32)
        lines = []
        for j in range(2):
            lines += [v[:, 128 * j : 128 * (j + 1)] for v in g] + [zero]
        lines = jnp.concatenate(lines, axis=0).astype(BF16)
        for s in range(8):
            msg[s, h, 0:32, :] = kv[32 * s : 32 * s + 32]
            a = q[h][32 * s : 32 * s + 16]
            b = q[h][32 * s + 16 : 32 * s + 32]
            msg[s, h, 32:48, :] = jnp.concatenate([a, b], axis=-1).astype(BF16)
            msg[s, h, 48:56, :] = lines
    copies[1].wait()
    pool[...] = dot_t(rows, wp[...]).astype(BF16)


def place(i, t):
    if t <= i:
        return i, (i, *range(i))[t], 0
    return 7 - i, t - i - 1, 1


def prepare_kernel(where, qy, gates, qs, side, mask):
    y, s = where[0], where[1]
    lane = iota((16, 128), 1)
    for z in range(NZ):
        for yy in range(NY):
            p = qy[yy, z].astype(F32)
            for half in range(2):
                base = half * 128 + yy * 32 + (z % 2) * 16
                q = p if half == 0 else pltpu.roll(p, 64, 1)
                qs[z // 2, base : base + 16, 0:128] = jnp.where(lane < 64, q, 0.0).astype(BF16)
    side[...] = gates[...].astype(F32).reshape(128, 128).T
    for m in range(8):
        qs[m, :, 128:256] = jnp.full((256, 128), -1.0, BF16)
    r = iota((512, 256), 0)
    l = iota((512, 256), 1)
    k_at = ((r // 256) * 4 + y) * 256 + r % 256
    q_at = (((l // 16) % 2) * 4 + (l // 32) % 4) * 256 + 32 * s + (l // 128) * 16 + l % 16
    mask[...] = jnp.where(k_at <= q_at, 0.0, NEG)


def attend_kernel(ks, qs, side, mask, out, kv, vt, buf_a, buf_b, lse):
    for z in range(NZ):
        for k in range(8):
            kv[z * 256 + 32 * k : z * 256 + 32 * k + 32, 0:128] = ks[k, z]
        for j in range(2):
            at = z * 256 + 128 * j
            mine = iota((128, 128), 1) // 4 == 2 * z + j
            kv[at : at + 128, 128:256] = jnp.where(mine, side[...], 0.0).astype(BF16)
            vt[:, at : at + 128] = kv[at : at + 128, 0:128].T[64:128]

    def logits_of(i, buf):
        tops = [None, None]
        for t in range(9):
            qi, j, k = place(i, t)
            v = dot_t(kv[512 * j : 512 * j + 512, :], qs[qi])
            if qi == j:
                v = v + mask[...]
            buf[t] = v
            m = jnp.max(v.reshape(64, 8, 256), axis=0)
            tops[k] = m if tops[k] is None else jnp.maximum(tops[k], m)
        return [jnp.maximum(jnp.max(m, axis=0, keepdims=True), -1e29) for m in tops]

    def weigh(i, buf, tops):
        sums, accs = [0.0, 0.0], [0.0, 0.0]
        for t in range(9):
            _, j, k = place(i, t)
            w = jnp.exp(buf[t] - tops[k])
            sums[k] = sums[k] + jnp.sum(w.reshape(64, 8, 256), axis=0)
            accs[k] = accs[k] + dot(vt[:, 512 * j : 512 * j + 512], w.astype(BF16))
        for k, m in ((0, i), (1, 7 - i)):
            n = jnp.sum(sums[k], axis=0, keepdims=True)
            some = n > 0.0
            safe = jnp.where(some, n, 1.0)
            lse[m : m + 1, :] = jnp.where(some, tops[k] + jnp.log(safe), NEG)
            o = accs[k] / safe
            o = jnp.concatenate([o[:, 0:128], o[:, 128:256]], axis=0).T.astype(BF16)
            for yy in range(NY):
                out[yy, 32 * m : 32 * m + 32, :] = o[32 * yy : 32 * yy + 32]

    bufs = (buf_a, buf_b)
    tops = logits_of(0, buf_a)
    for i in range(4):
        if i < 3:
            later = logits_of(i + 1, bufs[(i + 1) % 2])
        weigh(i, bufs[i % 2], tops)
        tops = later
    ln = iota((8, 128), 1)
    for yy in range(NY):
        a = pltpu.roll(lse[:, 0:128], (128 - 32 * yy) % 128, 1)
        b = pltpu.roll(lse[:, 128:256], (160 - 32 * yy) % 128, 1)
        v = jnp.where(ln < 32, a, jnp.where(ln < 64, b, 0.0))
        out[yy, 256:280, :] = jnp.concatenate(three_parts(v), axis=0).astype(BF16)


def merge_kernel(parts, out):
    lses = []
    for k in range(NY):
        v = parts[k, 256:280, :].astype(F32)
        lses.append(v[0:8] + v[8:16] + v[16:24])
    top = jnp.maximum(jnp.maximum(lses[0], lses[1]), jnp.maximum(lses[2], lses[3]))
    ws = [jnp.exp(v - top) for v in lses]
    den = (ws[0] + ws[1]) + (ws[2] + ws[3])
    ws = [(w / den).T for w in ws]
    half = iota((16, 128), 1) < 64
    for z in range(NZ):
        m, at = z // 2, (z % 2) * 16
        total = jnp.zeros((16, 128), F32)
        for k in range(NY):
            a = ws[k][at : at + 16, m : m + 1]
            b = ws[k][at + 32 : at + 48, m : m + 1]
            total = total + jnp.where(half, a, b) * parts[k, 16 * z : 16 * z + 16, :].astype(F32)
        out[z] = total.astype(BF16)


def pool_kernel(where, rim, cur, pooled):
    x, offset = where[0], where[1]
    now = cur[...].astype(F32)
    ext = jnp.concatenate([rim[...].astype(F32), now], axis=0)
    counts = (offset + iota((ROWS, 128), 0) + 1).astype(F32)
    mean = jnp.zeros((ROWS, 128), F32)
    run = ext
    for g in range(4):
        w = 2 ** (g + 1)
        n = run.shape[0]
        run = run[w // 2 :] + run[: n - w // 2]
        avg = run[run.shape[0] - ROWS :] / jnp.minimum(counts, float(w))
        mean = jnp.where(x == g, avg, mean)
    pooled[...] = (mean - now).astype(BF16)


def half_output(s_of, ref, wpo, wao, attended, total, start):
    half = iota((16, 128), 1) < 64
    for x in range(NX):
        rows = wpo[pl.ds(pl.multiple_of(s_of(x) * 128, 128), 128), :]
        start = start + dot(ref[x, 256:512, :], rows)
        for j in range(8):
            a = ref[x, 32 * j : 32 * j + 16, :].astype(F32)
            b = ref[x, 32 * j + 16 : 32 * j + 32, :].astype(F32)
            u = jnp.where(half, a, pltpu.roll(b, 64, 1)).astype(BF16)
            v = jnp.where(half, pltpu.roll(a, 64, 1), b).astype(BF16)
            attended[32 * x : 32 * x + 16, 128 * j : 128 * j + 128] = u
            attended[32 * x + 16 : 32 * x + 32, 128 * j : 128 * j + 128] = v
    total[...] = start
    mine = dot(attended[...], wao[...])
    for x in range(NX):
        at = pl.ds(pl.multiple_of(s_of(x) * SUB, SUB), SUB)
        total[at, :] = total[at, :] + mine[32 * x : 32 * x + 32]


def first_kernel(where, own, wpo, wao, total, attended):
    half_output(lambda x: 2 * x + where[0], own, wpo, wao, attended, total, 0.0)


def last_kernel(where, other, first, wpo, wao, out, attended, total):
    half_output(lambda x: 2 * x + 1 - where[0], other, wpo, wao, attended, total, first[...])
    out[...] = total[...].astype(BF16)


VM = pl.BlockSpec(memory_space=pltpu.VMEM)
SM = pl.BlockSpec(memory_space=pltpu.SMEM)


HB = pl.BlockSpec(memory_space=pltpu.HBM)


def call(kernel, where, ins, outs, scratch, flops, mib, in_hbm=()):
    head = [jnp.stack([jnp.asarray(w, jnp.int32) for w in where])] if where else []
    shapes = []
    for s in outs:
        wide = s[-1] == F32
        shapes.append(jax.ShapeDtypeStruct(s[:-1] if wide else s, F32 if wide else BF16))
    return pl.pallas_call(
        kernel,
        out_shape=shapes,
        in_specs=[SM] * len(head) + [HB if k in in_hbm else VM for k in range(len(ins))],
        out_specs=[VM] * len(outs),
        scratch_shapes=scratch,
        cost_estimate=pl.CostEstimate(flops=flops, bytes_accessed=2**20, transcendentals=0),
        compiler_params=pltpu.CompilerParams(vmem_limit_bytes=int(mib * 2**20)),
    )(*head, *ins)


def spread(value, axis):
    size = lax.axis_size(axis)
    copies = jnp.broadcast_to(value[None], (size, *value.shape))
    return lax.all_to_all(copies, axis, 0, 0, tiled=True)


def swap(value):
    return lax.ppermute(value, "c", [(0, 1), (1, 0)])


def layer(
    tokens, norm_gain, wq, wk, wv, wp, query_gain, key_gain, cum_gate, wpo, wao
):
    z, y, x, c = (lax.axis_index(a) for a in ("z", "y", "x", "c"))
    own = spread(tokens, "x")
    other = swap(own)
    (squares,) = call(early_kernel, (), (own,), [(ROWS, 128, F32)], [], 2**20, 4)
    msg, pool = call(
        project_kernel,
        (c,),
        (
            own,
            other,
            squares,
            norm_gain.reshape(1, 2048),
            wq,
            wk,
            wv,
            wp,
            query_gain.reshape(1, HEAD),
            key_gain.reshape(1, HEAD),
            cum_gate.T,
        ),
        [(8, 2, 56, 128), (ROWS, 128)],
        [pltpu.VMEM((ROWS, 2048), BF16)]
        + [pltpu.VMEM((128, 2048), BF16)] * 2
        + [pltpu.SemaphoreType.DMA((2,))],
        2 * ROWS * 2048 * 512,
        51.375,
        (6, 7),
    )
    count = NZ * NY
    heads = lax.all_to_all(msg.reshape(8, 112, 128), TP, 0, 0, tiled=True)
    mine = lax.all_to_all(heads.reshape(16, 56, 128), "z", 0, 0, tiled=True)
    ks = spread(mine[:, 0:32], TP)
    qy = lax.all_gather(mine[:, 32:48], "y", axis=0, tiled=False)
    qs, side, mask = call(
        prepare_kernel,
        (y, 2 * x + c),
        (qy, mine[:, 48:56]),
        [(8, 256, 256), (128, 128, F32), (512, 256, F32)],
        [],
        2**20,
        8,
    )
    (parts,) = call(
        attend_kernel,
        (),
        (ks, qs, side, mask),
        [(NY, 280, 128)],
        [
            pltpu.VMEM((4096, 256), BF16),
            pltpu.VMEM((64, 4096), BF16),
            pltpu.VMEM((9, 512, 256), F32),
            pltpu.VMEM((9, 512, 256), F32),
            pltpu.VMEM((8, 256), F32),
        ],
        4 * 72 * 256 * 256 * 128,
        28,
    )
    parts = lax.all_to_all(parts, "y", 0, 0, tiled=True)
    (merged,) = call(merge_kernel, (), (parts,), [(16, 16, 128)], [], 2**20, 8)
    rim = lax.ppermute(pool[ROWS - 16 :], SP, [(k, k + 1) for k in range(count - 1)])
    (pooled,) = call(
        pool_kernel, (x, (z * NY + y) * ROWS), (rim, pool), [(ROWS, 128)], [], 2**20, 4
    )
    back = lax.all_to_all(merged, "z", 0, 0, tiled=True)
    both = jnp.concatenate([back.reshape(256, 128), pooled], axis=0)
    own = spread(both, "x")
    other = swap(own)
    (first,) = call(
        first_kernel,
        (c,),
        (own, wpo, wao),
        [(ROWS, 256, F32)],
        [pltpu.VMEM((128, 1024), BF16)],
        ROWS * 2048 * 256,
        8,
    )
    (mixed,) = call(
        last_kernel,
        (c,),
        (other, first, wpo, wao),
        [(ROWS, 256)],
        [pltpu.VMEM((128, 1024), BF16), pltpu.VMEM((ROWS, 256), F32)],
        ROWS * 2048 * 256,
        8,
    )
    return mixed


def solution(mesh):
    grid = Mesh(mesh.devices.reshape(NZ, NY, NX, NC), ("z", "y", "x", "c"))
    return jax.shard_map(
        layer,
        mesh=grid,
        in_specs=(
            P(SP, TP),
            P(),
            P(TP, None),
            P(TP, None),
            P(TP, None),
            P(TP, None),
            P(),
            P(),
            P(SP, TP),
            P(None, TP),
            P(None, TP),
        ),
        out_specs=P(SP, TP),
        check_vma=False,
    )
```
